32 devices in a mesh: sp: 16 (over z, x, core), tp: 2 (over y).
Axes of the slice: x: 2, y: 2, z: 4, core: 2. Of those that a mesh axis runs over, the one named last changes fastest.
Arguments:
- skip_connection_stream: bfloat16 [12288, 2048], P('sp'), may hold values from -6 to 6
- probing_vectors: bfloat16 [12288, 512], P('sp', 'tp'), may hold values from -6 to 6
- addressing_vectors: bfloat16 [12288, 512], P('sp', 'tp'), may hold values from -6 to 6
- mapped_payloads: bfloat16 [12288, 1024], P('sp', 'tp'), may hold values from -6 to 6
- emission_switch: bfloat16 [12288, 1024], P('sp', 'tp'), may hold values from -6 to 6
- lapse_preactivation: bfloat16 [12288, 512], P('sp', 'tp')
- lapse_shift_entries: float32 [512], P('tp')
- surplus_attenuation_terms: float32 [12288], P('sp'), may hold values from -0.7 to 0
- passage_label_per_token: int32 [12288], P('sp'), may hold values from 0 to 3, never falling along the last dimension, each value on 1 to 6144 neighbouring positions
- attention_group_rescaler: float32 [128], replicated, may hold values from 0.1 to 1.9
- emission_projector: bfloat16 [1024, 2048], P('tp'), may hold values from -0.1875 to 0.1875
- perceptron_rescaler: float32 [2048], replicated, may hold values from 0.1 to 1.9
- switching_projector: bfloat16 [2048, 5632], P('sp', 'tp'), may hold values from -0.125 to 0.125
- widening_projector: bfloat16 [2048, 5632], P('sp', 'tp'), may hold values from -0.125 to 0.125
- shrinking_projector: bfloat16 [5632, 2048], P('tp', 'sp'), may hold values from -0.078125 to 0.078125
Outputs:
- layer_out: bfloat16 [12288, 2048], P(('sp', 'tp'))
The draws below stay inside these ranges and needn't reach their ends.
Inputs may be any that keep to these rules, and one draw needn't show every extreme that they name: `passage_label_per_token`: document numbers never fall along the sequence; a document holds at most 6144 positions.
All inputs are finite; a program needn't handle non-finite values.
Results may differ from the reference program's by a relative error of at most 0.014.
Values may be sent and summed in bfloat16 or wider, within the bound.
No kernel may reach another device: no remote copies, remote signals or barrier semaphores. Data moves between devices by JAX's collectives and lax.ppermute only.
A program may use at most 128 MiB of HBM per device.

```python
import math
import jax
import jax.numpy as jnp
import numpy as np
from jax import lax

D = 2048
HEADS = 8
DK = 64
DV = 128
FF = 5632
BLOCK = 64
TOK_DEV = 768
TOKENS = 12288
DOCS = 4
DOC_MOST = 6144
N_SP = 16
N_TP = 2


def draw_lapse_preactivation(key, part):
    base_key, block_key = jax.random.split(jax.random.fold_in(key, 11))
    width = HEADS * DK
    noise = jax.random.normal(base_key, (TOKENS, width), jnp.float32)
    shift = jax.random.uniform(block_key, (TOKENS // TOK_DEV, 1, width), jnp.float32, -0.7, 0.7)
    shaped = noise.reshape(TOKENS // TOK_DEV, TOK_DEV, width) + shift
    return shaped.reshape(TOKENS, width).astype(jnp.bfloat16)


def draw_lapse_shift_entries(key, part):
    pick_key, slow_key, fast_key = jax.random.split(jax.random.fold_in(key, 23), 3)
    slow = jax.random.randint(pick_key, (HEADS,), 0, 2) > 0
    slow_vals = jnp.log(TOKENS / 16.0) + jax.random.uniform(slow_key, (HEADS, DK), jnp.float32, -1.0, 0.5)
    fast_vals = jax.random.uniform(fast_key, (HEADS, DK), jnp.float32, -0.5, 1.5)
    return jnp.where(slow[:, None], slow_vals, fast_vals).reshape(HEADS * DK).astype(jnp.float32)


def draw_surplus_attenuation_terms(key, part):
    where_key, size_key = jax.random.split(jax.random.fold_in(key, 37))
    number = max(TOKENS // TOK_DEV, 4)
    spots = jax.random.randint(where_key, (number,), 0, TOKENS)
    depth = jnp.log(jax.random.uniform(size_key, (number,), jnp.float32, 0.5, 0.8))
    return jnp.zeros((TOKENS,), jnp.float32).at[spots].min(depth)


def steps_of(stream_key, shape, pieces, low, largest):
    def one(axis_at, shards_of):
        heights = jax.random.uniform(jax.random.fold_in(jax.random.fold_in(stream_key, 6), axis_at), (shards_of,), jnp.float32, low / len(pieces), largest / len(pieces))
        return jnp.repeat(jnp.exp(heights), shape[axis_at] // shards_of).reshape((-1,) + (1,) * (len(shape) - axis_at - 1))

    factor_of = one(*pieces[0])
    for cut in pieces[1:]:
        factor_of = factor_of * one(*cut)
    return factor_of


def profile(number_of, total, most, skew):
    portions = [(1 << 20) // math.isqrt(standing ** skew) + 1 for standing in range(2, number_of + 1)]
    surplus, holding = total - most - (number_of - 1), [1] * (number_of - 1)
    while surplus > 0:
        movable = [i for i in range(number_of - 1) if holding[i] < most]
        mass, remaining = sum([portions[i] for i in movable]), surplus
        for i in movable:
            extra = min(most - holding[i], max(1, remaining * portions[i] // mass), surplus)
            holding[i] = holding[i] + extra
            surplus = surplus - extra
    return np.array([most] + holding)


def uneven(rng, number_of, total, limit, skew):
    if number_of == 2:
        one = jax.random.randint(rng, (), max(1, total - limit), min(limit, total - 1) + 1)
        return jnp.stack([one, total - one])
    lengths = jnp.asarray(profile(number_of, total, limit, skew), jnp.int32)
    twos = (number_of - 1) // 2
    giver, receiver = lengths[1:1 + 2 * twos:2], lengths[2:2 + 2 * twos:2]
    slack = jnp.minimum(giver - 1, limit - receiver)
    passed = jax.random.randint(jax.random.fold_in(rng, 1), (twos,), 0, 1 << 20) % (slack + 1)
    lengths = lengths.at[1:1 + 2 * twos:2].set(giver - passed).at[2:2 + 2 * twos:2].set(receiver + passed)
    return lengths[jax.random.permutation(jax.random.fold_in(rng, 2), number_of)]


def scatter_about(own_key, shape, scale, reach, cuts=(), kind=jnp.bfloat16):
    drawn = scale * jax.random.normal(own_key, shape, jnp.float32)
    if cuts:
        drawn = drawn * steps_of(own_key, shape, cuts, -0.22, 0.18)
    return jnp.clip(drawn, -reach, reach).astype(kind)


def setup_inputs(seed: int = 0) -> dict:
    splits = jax.random.split(jax.random.key(seed), 16)
    skip_connection_stream = scatter_about(splits[0], (TOKENS, D), 1.0, 6.0, ((0, 16),))
    probing_vectors = scatter_about(splits[1], (TOKENS, HEADS * DK), 1.0, 6.0, ((0, 16), (1, 2)))
    addressing_vectors = scatter_about(splits[2], (TOKENS, HEADS * DK), 1.0, 6.0, ((0, 16), (1, 2)))
    mapped_payloads = scatter_about(splits[3], (TOKENS, HEADS * DV), 1.0, 6.0, ((0, 16), (1, 2)))
    emission_switch = scatter_about(splits[4], (TOKENS, HEADS * DV), 1.0, 6.0, ((0, 16), (1, 2)))
    lapse_preactivation = draw_lapse_preactivation(jax.random.fold_in(splits[15], 71), 0)
    lapse_shift_entries = draw_lapse_shift_entries(jax.random.fold_in(splits[15], 71), 0)
    surplus_attenuation_terms = draw_surplus_attenuation_terms(jax.random.fold_in(splits[15], 71), 0)
    passage_label_per_token = jnp.searchsorted(jnp.cumsum(uneven(splits[8], DOCS, TOKENS, DOC_MOST, 1)), jnp.arange(TOKENS), side="right").astype(jnp.int32)
    attention_group_rescaler = jnp.clip(1.0 + 0.18 * jax.random.normal(splits[9], (DV,), jnp.float32), 0.1, 1.9)
    emission_projector = scatter_about(splits[10], (HEADS * DV, D), (HEADS * DV) ** -0.5, 0.1875, ((0, 2),))
    perceptron_rescaler = jnp.clip(1.0 + 0.18 * jax.random.normal(splits[11], (D,), jnp.float32), 0.1, 1.9)
    switching_projector = scatter_about(splits[12], (D, FF), D ** -0.5, 0.125, ((0, 16), (1, 2)))
    widening_projector = scatter_about(splits[13], (D, FF), D ** -0.5, 0.125, ((0, 16), (1, 2)))
    shrinking_projector = scatter_about(splits[14], (FF, D), FF ** -0.5, 0.078125, ((0, 2), (1, 16)))
    return {"skip_connection_stream": skip_connection_stream, "probing_vectors": probing_vectors, "addressing_vectors": addressing_vectors, "mapped_payloads": mapped_payloads, "emission_switch": emission_switch, "lapse_preactivation": lapse_preactivation, "lapse_shift_entries": lapse_shift_entries, "surplus_attenuation_terms": surplus_attenuation_terms, "passage_label_per_token": passage_label_per_token, "attention_group_rescaler": attention_group_rescaler, "emission_projector": emission_projector, "perceptron_rescaler": perceptron_rescaler, "switching_projector": switching_projector, "widening_projector": widening_projector, "shrinking_projector": shrinking_projector}


eps = 1e-06
sharpness_factor = 16.0

def head_split(array, heads):
    return array.reshape(array.shape[0], heads, -1).transpose(1, 0, 2)

def rounded(value):
    return lax.optimization_barrier(value.astype(jnp.bfloat16)).astype(jnp.float32)

def block_pass(query_head_rows, key_heads, value_heads, decay_heads, documents, recurrent_state, last_doc, offset, span):
    heads, length, _ = query_head_rows.shape
    blocks = length // span

    def to_blocks(array):
        return array.reshape(heads, blocks, span, array.shape[-1]).transpose(1, 0, 2, 3)
    lower = jnp.tril(jnp.ones((span, span), dtype=bool))

    def step(carry, inputs):
        recurrent_state, last_doc, offset = carry
        query_block, key_blk, value_block, piece_attenuation, doc_blk = inputs
        cumulative_decay = jnp.cumsum(piece_attenuation, axis=1)
        previous_valid = (doc_blk == last_doc).astype(jnp.float32)
        cross_block_output = jnp.einsum('gfl,glm->gfm', query_block * jnp.exp(cumulative_decay), recurrent_state, precision=lax.Precision.HIGHEST) * previous_valid[None, :, None]
        spread = cumulative_decay[:, :, None, :] - cumulative_decay[:, None, :, :]
        same = (doc_blk[:, None] == doc_blk[None, :]) & lower
        weights = jnp.exp(jnp.where(same[None, :, :, None], spread, -jnp.inf))
        scores = jnp.einsum('hik,hjk,hijk->hij', query_block, key_blk, weights, precision=lax.Precision.HIGHEST)
        result = cross_block_output + jnp.einsum('hij,hjv->hiv', scores, value_block, precision=lax.Precision.HIGHEST)
        final_memory_summary = cumulative_decay[:, -1, :]
        last_valid = (doc_blk[-1] == last_doc).astype(jnp.float32)
        tail_ok = (doc_blk == doc_blk[-1]).astype(jnp.float32)
        decayed_keys = key_blk * jnp.exp(final_memory_summary[:, None, :] - cumulative_decay) * tail_ok[None, :, None]
        recurrent_state = recurrent_state * jnp.exp(final_memory_summary)[:, :, None] * last_valid + jnp.einsum('wrz,wrs->wzs', decayed_keys, value_block, precision=lax.Precision.HIGHEST)
        return ((recurrent_state, doc_blk[-1], offset + final_memory_summary), (result, cumulative_decay + offset[:, None, :]))
    carry, outputs = lax.scan(step, (recurrent_state, last_doc, offset), (to_blocks(query_head_rows), to_blocks(key_heads), to_blocks(value_heads), to_blocks(decay_heads), documents.reshape(blocks, span)))
    result, running_state = outputs
    result = result.transpose(1, 0, 2, 3).reshape(heads, length, -1)
    running_state = running_state.transpose(1, 0, 2, 3).reshape(heads, length, -1)
    return (carry[0], carry[2], result, running_state)

def reference(skip_connection_stream, probing_vectors, addressing_vectors, mapped_payloads, emission_switch, lapse_preactivation, lapse_shift_entries, surplus_attenuation_terms, passage_label_per_token, attention_group_rescaler, emission_projector, perceptron_rescaler, switching_projector, widening_projector, shrinking_projector):
    keeping_exponent = jax.nn.log_sigmoid(lapse_preactivation.astype(jnp.float32) + lapse_shift_entries[None, :]) / sharpness_factor + surplus_attenuation_terms[:, None]
    query_head_rows = head_split(probing_vectors.astype(jnp.float32) * DK ** (-0.5), HEADS)
    key_heads = head_split(addressing_vectors.astype(jnp.float32), HEADS)
    value_heads = head_split(mapped_payloads.astype(jnp.float32), HEADS)
    decay_heads = head_split(keeping_exponent, HEADS)
    zero_state = jnp.zeros((HEADS, DK, DV), jnp.float32)
    _, _, attn, _ = block_pass(query_head_rows, key_heads, value_heads, decay_heads, passage_label_per_token, zero_state, jnp.array(-1, jnp.int32), jnp.zeros((HEADS, DK), jnp.float32), BLOCK)
    normed_attn = attn * lax.rsqrt(lax.optimization_barrier(jnp.mean(attn * attn, axis=-1, keepdims=True)) + eps) * attention_group_rescaler
    flat = normed_attn.transpose(1, 0, 2).reshape(attn.shape[1], HEADS * DV)
    gated = (flat * jax.nn.silu(emission_switch.astype(jnp.float32))).astype(jnp.bfloat16)
    head_cols = HEADS * DV // N_TP
    ff_cols = FF // N_TP

    def rows_fn(index):
        start = (index * TOK_DEV).astype(jnp.int32)
        gated_rows = lax.dynamic_slice_in_dim(gated, start, TOK_DEV, 0)
        resid_rows = lax.dynamic_slice_in_dim(skip_connection_stream, start, TOK_DEV, 0)
        mixed = jnp.zeros((TOK_DEV, D), jnp.float32)
        for group in range(N_TP):
            mixed = mixed + rounded(jnp.dot(gated_rows[:, group * head_cols:(group + 1) * head_cols], emission_projector[group * head_cols:(group + 1) * head_cols], preferred_element_type=jnp.float32))
        first_resid = (resid_rows.astype(jnp.float32) + mixed).astype(jnp.bfloat16)
        wide = first_resid.astype(jnp.float32)
        normed = (wide * lax.rsqrt(lax.optimization_barrier(jnp.mean(wide * wide, axis=-1, keepdims=True)) + eps) * perceptron_rescaler).astype(jnp.bfloat16)
        gate = jnp.dot(normed, switching_projector, preferred_element_type=jnp.float32)
        upper = jnp.dot(normed, widening_projector, preferred_element_type=jnp.float32)
        hidden = (jax.nn.silu(gate) * upper).astype(jnp.bfloat16)
        ffn_out = jnp.zeros((TOK_DEV, D), jnp.float32)
        for group in range(N_TP):
            ffn_out = ffn_out + rounded(jnp.dot(hidden[:, group * ff_cols:(group + 1) * ff_cols], shrinking_projector[group * ff_cols:(group + 1) * ff_cols], preferred_element_type=jnp.float32))
        return (wide + 0.5 * ffn_out).astype(jnp.bfloat16)
    blocks_out = lax.map(rows_fn, jnp.arange(N_SP, dtype=jnp.int32))
    return blocks_out.reshape(N_SP * TOK_DEV, D)
```

```python
import jax
import jax.numpy as jnp
from jax import lax
from jax.experimental import pallas as pl
from jax.experimental.pallas import tpu as pltpu
from jax.sharding import PartitionSpec as P

DK = 64
DV = 128
BLOCK = 64

eps = 1e-06
sharpness_factor = 16.0

NN = (((1,), (0,)), ((), ()))
NT = (((1,), (1,)), ((), ()))
TN = (((0,), (0,)), ((), ()))


def mm(a, b, dims):
    return lax.dot_general(
        a.astype(jnp.bfloat16), b.astype(jnp.bfloat16), dims, preferred_element_type=jnp.float32
    )


def local_kernel(
    q_ref, k_ref, v_ref, f_ref, shift_ref, extra_ref, doc_ref, docrow_ref,
    out_ref, qrun_ref, state_ref, total_ref, ld_ref,
):
    rows, width = q_ref.shape
    pairs = width // (2 * DK)
    blocks = rows // BLOCK
    pre = f_ref[...].astype(jnp.float32) + shift_ref[...]
    ld_ref[...] = (
        jnp.minimum(pre, 0.0) - jnp.log1p(jnp.exp(-jnp.abs(pre)))
    ) / sharpness_factor + extra_ref[...]
    r = lax.broadcasted_iota(jnp.int32, (BLOCK, BLOCK), 0)
    c = lax.broadcasted_iota(jnp.int32, (BLOCK, BLOCK), 1)
    lower = c <= r
    tril = lower.astype(jnp.float32)
    half = lax.broadcasted_iota(jnp.int32, (BLOCK, 2 * DK), 1) < DK
    sr = lax.broadcasted_iota(jnp.int32, (2 * DK, 2 * DV), 0) < DK
    sc = lax.broadcasted_iota(jnp.int32, (2 * DK, 2 * DV), 1) < DV
    diag = sr == sc
    state = [jnp.zeros((2 * DK, 2 * DV), jnp.float32) for _ in range(pairs)]
    offset = jnp.zeros((1, width), jnp.float32)
    last = doc_ref[0:1, :]
    for b in range(blocks):
        at = slice(b * BLOCK, (b + 1) * BLOCK)
        cum = lax.dot_general(
            tril, ld_ref[at, :], NN, precision=lax.Precision.HIGHEST,
            preferred_element_type=jnp.float32,
        )
        doc = doc_ref[at, :]
        docrow = docrow_ref[b : b + 1, :]
        end = doc_ref[(b + 1) * BLOCK - 1 : (b + 1) * BLOCK, :]
        same = (doc == docrow) & lower
        prev_ok = (doc == last).astype(jnp.float32)
        tail_ok = (doc == end).astype(jnp.float32)
        last_ok = (end == last).astype(jnp.float32)
        q = q_ref[at, :].astype(jnp.float32) * DK ** (-0.5)
        k = k_ref[at, :].astype(jnp.float32)
        final = cum[BLOCK - 1 : BLOCK, :]
        centre = cum[BLOCK // 2 : BLOCK // 2 + 1, :]
        qe = q * jnp.exp(cum)
        qs = q * jnp.exp(cum - centre)
        ks = (k * jnp.exp(centre - cum)).astype(jnp.bfloat16)
        kd = k * jnp.exp(final - cum) * tail_ok
        qrun_ref[at, :] = (qe * jnp.exp(offset)).astype(jnp.bfloat16)
        fall = jnp.exp(final) * last_ok
        for p in range(pairs):
            kk = slice(p * 2 * DK, (p + 1) * 2 * DK)
            vv = slice(p * 2 * DV, (p + 1) * 2 * DV)
            v = v_ref[at, vv]
            cross = mm(qe[:, kk], state[p], NN) * prev_ok
            sa = mm(jnp.where(half, qs[:, kk], 0.0), ks[:, kk], NT)
            sb = mm(jnp.where(half, 0.0, qs[:, kk]), ks[:, kk], NT)
            oa = mm(jnp.where(same, sa, 0.0), v[:, :DV], NN)
            ob = mm(jnp.where(same, sb, 0.0), v[:, DV:], NN)
            out_ref[at, vv] = cross + jnp.concatenate([oa, ob], axis=1)
            fresh = mm(kd[:, kk], v, TN)
            decay = jnp.transpose(jnp.broadcast_to(fall[:, kk], (8, 2 * DK)))[:, 0:1]
            state[p] = state[p] * decay + jnp.where(diag, fresh, 0.0)
        offset = offset + final
        last = end
    for p in range(pairs):
        state_ref[(2 * p) * DK : (2 * p + 1) * DK, :] = state[p][:DK, :DV].astype(jnp.bfloat16)
        state_ref[(2 * p + 1) * DK : (2 * p + 2) * DK, :] = state[p][DK:, DV:].astype(jnp.bfloat16)
    total_ref[...] = offset


def finish_kernel(out_ref, qrun_ref, state_ref, reach_ref, gain_ref, gate_ref, gated_ref):
    heads = out_ref.shape[1] // DV
    reach = reach_ref[...]
    gain = gain_ref[...]
    for h in range(heads):
        p = h // 2
        q = qrun_ref[:, p * 2 * DK : (p + 1) * 2 * DK]
        s = state_ref[p * 2 * DK : (p + 1) * 2 * DK, :]
        keep = (lax.broadcasted_iota(jnp.int32, s.shape, 0) < DK) == (h % 2 == 0)
        s = jnp.where(keep, s, 0.0)
        vv = slice(h * DV, (h + 1) * DV)
        attn = out_ref[:, vv] + mm(q, s, NN) * reach
        mean = jnp.mean(attn * attn, axis=-1, keepdims=True)
        g = gate_ref[:, vv].astype(jnp.float32)
        gated_ref[:, vv] = (
            attn * lax.rsqrt(mean + eps) * gain * (g / (1.0 + jnp.exp(-g)))
        ).astype(jnp.bfloat16)


def rms_rows(rows, gain):
    wide = rows.astype(jnp.float32)
    return (wide * lax.rsqrt(jnp.mean(wide * wide, axis=-1, keepdims=True) + eps) * gain).astype(
        jnp.bfloat16
    )


def shift(a, axis, k):
    n = lax.axis_size(axis)
    return lax.ppermute(a, axis, [(i, (i + k) % n) for i in range(n)])


def carried(state, decay, first, final, heads):
    n = lax.axis_size("sp")
    place = lax.axis_index("sp")
    states = lax.all_gather(state, "sp")
    small = jnp.concatenate(
        [
            decay.reshape(heads, DK),
            jnp.full((1, DK), first, jnp.float32),
            jnp.full((1, DK), final, jnp.float32),
        ],
        axis=0,
    ).astype(jnp.bfloat16)
    smalls = lax.all_gather(small, "sp").astype(jnp.float32)
    decays = smalls[:, :heads].reshape(n, heads * DK)
    firsts = smalls[:, heads, 0]
    finals = smalls[:, heads + 1, 0]
    linked = jnp.concatenate([jnp.zeros((1,)), (finals[:-1] == firsts[1:]).astype(jnp.float32)])
    run = jnp.ones((heads * DK,), jnp.float32)
    total = jnp.zeros(state.shape, jnp.float32)
    for j in reversed(range(n)):
        before = j < place
        total = total + jnp.where(before, run, 0.0)[:, None] * states[j].astype(jnp.float32)
        run = jnp.where(before, run * decays[j] * linked[j], run)
    doc = jnp.where(place > 0, lax.dynamic_index_in_dim(finals, jnp.maximum(place - 1, 0), 0, False), -1.0)
    return total, doc


def per_device(
    skip_connection_stream,
    probing_vectors,
    addressing_vectors,
    mapped_payloads,
    emission_switch,
    lapse_preactivation,
    lapse_shift_entries,
    surplus_attenuation_terms,
    passage_label_per_token,
    attention_group_rescaler,
    emission_projector,
    perceptron_rescaler,
    switching_projector,
    widening_projector,
    shrinking_projector,
):
    rows, width = probing_vectors.shape
    heads = width // DK
    tp = lax.axis_size("tp")
    mine = lax.axis_index("tp")

    switching = lax.all_gather(switching_projector, "sp", axis=0, tiled=True)
    widening = lax.all_gather(widening_projector, "sp", axis=0, tiled=True)
    shrinking = lax.all_gather(shrinking_projector, "sp", axis=1, tiled=True)
    projectors = [emission_projector] + [shift(emission_projector, "tp", k) for k in range(1, tp)]

    docs = passage_label_per_token
    f32 = jnp.float32
    local_out, qrun, state, total = pl.pallas_call(
        local_kernel,
        out_shape=(
            jax.ShapeDtypeStruct((rows, heads * DV), f32),
            jax.ShapeDtypeStruct((rows, width), jnp.bfloat16),
            jax.ShapeDtypeStruct((heads * DK, DV), jnp.bfloat16),
            jax.ShapeDtypeStruct((1, width), f32),
        ),
        scratch_shapes=[pltpu.VMEM((rows, width), f32)],
        name="local_pass",
    )(
        probing_vectors,
        addressing_vectors,
        mapped_payloads,
        lapse_preactivation,
        lapse_shift_entries[None, :],
        surplus_attenuation_terms[:, None],
        docs[:, None],
        docs.reshape(rows // BLOCK, BLOCK),
    )
    first = docs[0].astype(f32)
    final = docs[-1].astype(f32)
    unbroken = (first == final).astype(f32)
    state_in, doc_in = carried(state, jnp.exp(total[0]) * unbroken, first, final, heads)
    reach = (docs.astype(f32) == doc_in).astype(f32)[:, None]
    gated = pl.pallas_call(
        finish_kernel,
        out_shape=jax.ShapeDtypeStruct((rows, heads * DV), jnp.bfloat16),
        name="finish_pass",
    )(local_out, qrun, state_in, reach, attention_group_rescaler[None, :], emission_switch)

    others = [gated] + [shift(gated, "tp", k) for k in range(1, tp)]
    mixed = jnp.zeros((rows, skip_connection_stream.shape[1]), f32)
    for g, w in zip(others, projectors):
        mixed = mixed + jnp.dot(g, w, preferred_element_type=f32)
    first_all = (skip_connection_stream.astype(f32) + mixed).astype(jnp.bfloat16)
    normed = rms_rows(first_all, perceptron_rescaler)
    gate = jnp.dot(normed, switching, preferred_element_type=f32)
    upper = jnp.dot(normed, widening, preferred_element_type=f32)
    hidden = (jax.nn.silu(gate) * upper).astype(jnp.bfloat16)

    share = rows // tp
    parts = 2
    step = share // parts
    arrived = []
    for k in range(1, tp):
        start = ((mine + k) % tp) * share
        for i in range(parts):
            sent = jnp.dot(
                lax.dynamic_slice_in_dim(hidden, start + i * step, step, 0),
                shrinking,
                preferred_element_type=f32,
            ).astype(jnp.bfloat16)
            arrived.append((i, shift(sent, "tp", k)))
    own = jnp.dot(
        lax.dynamic_slice_in_dim(hidden, mine * share, share, 0),
        shrinking,
        preferred_element_type=f32,
    )
    first_own = lax.dynamic_slice_in_dim(first_all, mine * share, share, 0).astype(f32)
    outs = []
    for i in range(parts):
        at = slice(i * step, (i + 1) * step)
        ffn = own[at].astype(jnp.bfloat16).astype(f32)
        for j, piece in arrived:
            if j == i:
                ffn = ffn + piece.astype(f32)
        outs.append((first_own[at] + 0.5 * ffn).astype(jnp.bfloat16))
    return jnp.concatenate(outs, axis=0)


def solution(mesh):
    placed = (
        P("sp", None),
        P("sp", "tp"),
        P("sp", "tp"),
        P("sp", "tp"),
        P("sp", "tp"),
        P("sp", "tp"),
        P("tp"),
        P("sp"),
        P("sp"),
        P(),
        P("tp", None),
        P(),
        P("sp", "tp"),
        P("sp", "tp"),
        P("tp", "sp"),
    )
    return jax.shard_map(
        per_device, mesh=mesh, in_specs=placed, out_specs=P(("sp", "tp"), None), check_vma=False
    )
```

```python
import math

import jax
import jax.numpy as jnp
from jax import lax
from jax.experimental import pallas as pl
from jax.experimental.pallas import tpu as pltpu
from jax.sharding import PartitionSpec as P

DK = 64
DV = 128
BLOCK = 64

eps = 1e-06
sharpness_factor = 16.0

NN = (((1,), (0,)), ((), ()))
NT = (((1,), (1,)), ((), ()))
TN = (((0,), (0,)), ((), ()))


def mm(a, b, dims):
    return lax.dot_general(
        a.astype(jnp.bfloat16), b.astype(jnp.bfloat16), dims, preferred_element_type=jnp.float32
    )


def local_kernel(
    q_ref, k_ref, v_ref, f_ref, shift_ref, extra_ref, doc_ref, docrow_ref,
    out_ref, qrun_ref, state_ref, total_ref, ld_ref,
):
    rows, width = q_ref.shape
    pairs = width // (2 * DK)
    blocks = rows // BLOCK
    pre = f_ref[...].astype(jnp.float32) + shift_ref[...]
    ld_ref[...] = (
        jnp.minimum(pre, 0.0) - jnp.log1p(jnp.exp(-jnp.abs(pre)))
    ) / sharpness_factor + extra_ref[...]
    r = lax.broadcasted_iota(jnp.int32, (BLOCK, BLOCK), 0)
    c = lax.broadcasted_iota(jnp.int32, (BLOCK, BLOCK), 1)
    lower = c <= r
    tril = lower.astype(jnp.float32)
    half = lax.broadcasted_iota(jnp.int32, (BLOCK, 2 * DK), 1) < DK
    sr = lax.broadcasted_iota(jnp.int32, (2 * DK, 2 * DV), 0) < DK
    sc = lax.broadcasted_iota(jnp.int32, (2 * DK, 2 * DV), 1) < DV
    diag = sr == sc
    state = [jnp.zeros((2 * DK, 2 * DV), jnp.float32) for _ in range(pairs)]
    offset = jnp.zeros((1, width), jnp.float32)
    last = doc_ref[0:1, :]
    for b in range(blocks):
        at = slice(b * BLOCK, (b + 1) * BLOCK)
        cum = lax.dot_general(
            tril, ld_ref[at, :], NN, precision=lax.Precision.HIGHEST,
            preferred_element_type=jnp.float32,
        )
        doc = doc_ref[at, :]
        docrow = docrow_ref[b : b + 1, :]
        end = doc_ref[(b + 1) * BLOCK - 1 : (b + 1) * BLOCK, :]
        same = (doc == docrow) & lower
        prev_ok = (doc == last).astype(jnp.float32)
        tail_ok = (doc == end).astype(jnp.float32)
        last_ok = (end == last).astype(jnp.float32)
        q = q_ref[at, :].astype(jnp.float32) * DK ** (-0.5)
        k = k_ref[at, :].astype(jnp.float32)
        final = cum[BLOCK - 1 : BLOCK, :]
        centre = cum[BLOCK // 2 : BLOCK // 2 + 1, :]
        qe = q * jnp.exp(cum)
        qs = q * jnp.exp(cum - centre)
        ks = (k * jnp.exp(centre - cum)).astype(jnp.bfloat16)
        kd = k * jnp.exp(final - cum) * tail_ok
        qrun_ref[at, :] = (qe * jnp.exp(offset)).astype(jnp.bfloat16)
        fall = jnp.exp(final) * last_ok
        for p in range(pairs):
            kk = slice(p * 2 * DK, (p + 1) * 2 * DK)
            vv = slice(p * 2 * DV, (p + 1) * 2 * DV)
            v = v_ref[at, vv]
            cross = mm(qe[:, kk], state[p], NN) * prev_ok
            sa = mm(jnp.where(half, qs[:, kk], 0.0), ks[:, kk], NT)
            sb = mm(jnp.where(half, 0.0, qs[:, kk]), ks[:, kk], NT)
            oa = mm(jnp.where(same, sa, 0.0), v[:, :DV], NN)
            ob = mm(jnp.where(same, sb, 0.0), v[:, DV:], NN)
            out_ref[at, vv] = cross + jnp.concatenate([oa, ob], axis=1)
            fresh = mm(kd[:, kk], v, TN)
            decay = jnp.transpose(jnp.broadcast_to(fall[:, kk], (8, 2 * DK)))[:, 0:1]
            state[p] = state[p] * decay + jnp.where(diag, fresh, 0.0)
        offset = offset + final
        last = end
    for p in range(pairs):
        state_ref[(2 * p) * DK : (2 * p + 1) * DK, :] = state[p][:DK, :DV].astype(jnp.bfloat16)
        state_ref[(2 * p + 1) * DK : (2 * p + 2) * DK, :] = state[p][DK:, DV:].astype(jnp.bfloat16)
    total_ref[...] = offset


def finish_kernel(out_ref, qrun_ref, state_ref, reach_ref, gain_ref, gate_ref, gated_ref):
    heads = out_ref.shape[1] // DV
    reach = reach_ref[...]
    gain = gain_ref[...]
    for h in range(heads):
        p = h // 2
        q = qrun_ref[:, p * 2 * DK : (p + 1) * 2 * DK]
        s = state_ref[p * 2 * DK : (p + 1) * 2 * DK, :]
        keep = (lax.broadcasted_iota(jnp.int32, s.shape, 0) < DK) == (h % 2 == 0)
        s = jnp.where(keep, s, 0.0)
        vv = slice(h * DV, (h + 1) * DV)
        attn = out_ref[:, vv] + mm(q, s, NN) * reach
        mean = jnp.mean(attn * attn, axis=-1, keepdims=True)
        g = gate_ref[:, vv].astype(jnp.float32)
        gated_ref[:, vv] = (
            attn * lax.rsqrt(mean + eps) * gain * (g / (1.0 + jnp.exp(-g)))
        ).astype(jnp.bfloat16)


def rms_rows(rows, gain):
    wide = rows.astype(jnp.float32)
    return (wide * lax.rsqrt(jnp.mean(wide * wide, axis=-1, keepdims=True) + eps) * gain).astype(
        jnp.bfloat16
    )


def shift(a, axis, k):
    n = lax.axis_size(axis)
    return lax.ppermute(a, axis, [(i, (i + k) % n) for i in range(n)])


def factors(n):
    lanes = max(math.isqrt(n // 4), 1)
    if n % (2 * lanes):
        return n, 1, 1
    return n // (2 * lanes), lanes, 2


def move(a, dim, k):
    n = lax.axis_size("sp")
    sizes = factors(n)
    pairs = []
    for i in range(n):
        at = [i // (sizes[1] * sizes[2]), i // sizes[2] % sizes[1], i % sizes[2]]
        at[dim] = (at[dim] + k) % sizes[dim]
        pairs.append((i, (at[0] * sizes[1] + at[1]) * sizes[2] + at[2]))
    return lax.ppermute(a, "sp", pairs)


def spread(shard, axis):
    planes, lanes, cores = factors(lax.axis_size("sp"))
    line = [shard] + [move(shard, 0, k) for k in range(1, planes)]
    blocks = []
    for block in line:
        blocks.append(block)
        blocks.extend(move(block, 1, k) for k in range(1, lanes))
    near = jnp.concatenate(blocks, axis=axis)
    return [near] + [move(near, 2, k) for k in range(1, cores)]


def turned(a, dim, k):
    n = a.shape[dim]
    if n == 1:
        return a
    return lax.dynamic_slice_in_dim(jnp.concatenate([a, a], axis=dim), k % n, n, dim)


def place_of():
    planes, lanes, cores = factors(lax.axis_size("sp"))
    i = lax.axis_index("sp")
    return i // (lanes * cores), i // cores % lanes, i % cores


def to_offsets(rows):
    sizes = factors(lax.axis_size("sp"))
    z, x, c = place_of()
    a = rows.reshape(rows.shape[0], *sizes, -1)
    a = turned(a[:, ::-1], 1, sizes[0] - 1 - z)
    a = turned(a[:, :, ::-1], 2, sizes[1] - 1 - x)
    a = turned(a[:, :, :, ::-1], 3, sizes[2] - 1 - c)
    return [a[:, :, :, k].reshape(rows.shape[0], -1) for k in range(sizes[2])]


def from_offsets(parts):
    sizes = factors(lax.axis_size("sp"))
    z, x, c = place_of()
    rows = parts[0].shape[0]
    a = jnp.stack([p.reshape(rows, sizes[0], sizes[1], -1) for p in parts], axis=3)
    a = turned(a, 1, z + 1)[:, ::-1]
    a = turned(a, 2, x + 1)[:, :, ::-1]
    a = turned(a, 3, c + 1)[:, :, :, ::-1]
    return a.reshape(rows, -1)


def joined(rows, weights):
    total = jnp.dot(rows[0], weights[0], preferred_element_type=jnp.float32)
    for r, w in zip(rows[1:], weights[1:]):
        total = total + jnp.dot(r, w, preferred_element_type=jnp.float32)
    return total


def carried(state, decay, first, final, heads):
    n = lax.axis_size("sp")
    place = lax.axis_index("sp")
    states = lax.all_gather(state, "sp")
    small = jnp.concatenate(
        [
            decay.reshape(heads, DK),
            jnp.full((1, DK), first, jnp.float32),
            jnp.full((1, DK), final, jnp.float32),
        ],
        axis=0,
    ).astype(jnp.bfloat16)
    smalls = lax.all_gather(small, "sp").astype(jnp.float32)
    decays = smalls[:, :heads].reshape(n, heads * DK)
    firsts = smalls[:, heads, 0]
    finals = smalls[:, heads + 1, 0]
    linked = jnp.concatenate([jnp.zeros((1,)), (finals[:-1] == firsts[1:]).astype(jnp.float32)])
    run = jnp.ones((heads * DK,), jnp.float32)
    total = jnp.zeros(state.shape, jnp.float32)
    for j in reversed(range(n)):
        before = j < place
        total = total + jnp.where(before, run, 0.0)[:, None] * states[j].astype(jnp.float32)
        run = jnp.where(before, run * decays[j] * linked[j], run)
    doc = jnp.where(place > 0, lax.dynamic_index_in_dim(finals, jnp.maximum(place - 1, 0), 0, False), -1.0)
    return total, doc


def per_device(
    skip_connection_stream,
    probing_vectors,
    addressing_vectors,
    mapped_payloads,
    emission_switch,
    lapse_preactivation,
    lapse_shift_entries,
    surplus_attenuation_terms,
    passage_label_per_token,
    attention_group_rescaler,
    emission_projector,
    perceptron_rescaler,
    switching_projector,
    widening_projector,
    shrinking_projector,
):
    rows, width = probing_vectors.shape
    heads = width // DK
    tp = lax.axis_size("tp")
    mine = lax.axis_index("tp")

    switching = [lax.all_gather(switching_projector, "sp", axis=0, tiled=True)]
    widening = spread(widening_projector, 0)
    shrinking = [lax.all_gather(shrinking_projector, "sp", axis=1, tiled=True)]
    projectors = [emission_projector] + [shift(emission_projector, "tp", k) for k in range(1, tp)]

    docs = passage_label_per_token
    f32 = jnp.float32
    local_out, qrun, state, total = pl.pallas_call(
        local_kernel,
        out_shape=(
            jax.ShapeDtypeStruct((rows, heads * DV), f32),
            jax.ShapeDtypeStruct((rows, width), jnp.bfloat16),
            jax.ShapeDtypeStruct((heads * DK, DV), jnp.bfloat16),
            jax.ShapeDtypeStruct((1, width), f32),
        ),
        scratch_shapes=[pltpu.VMEM((rows, width), f32)],
        name="local_pass",
    )(
        probing_vectors,
        addressing_vectors,
        mapped_payloads,
        lapse_preactivation,
        lapse_shift_entries[None, :],
        surplus_attenuation_terms[:, None],
        docs[:, None],
        docs.reshape(rows // BLOCK, BLOCK),
    )
    first = docs[0].astype(f32)
    final = docs[-1].astype(f32)
    unbroken = (first == final).astype(f32)
    state_in, doc_in = carried(state, jnp.exp(total[0]) * unbroken, first, final, heads)
    reach = (docs.astype(f32) == doc_in).astype(f32)[:, None]
    gated = pl.pallas_call(
        finish_kernel,
        out_shape=jax.ShapeDtypeStruct((rows, heads * DV), jnp.bfloat16),
        name="finish_pass",
    )(local_out, qrun, state_in, reach, attention_group_rescaler[None, :], emission_switch)

    others = [gated] + [shift(gated, "tp", k) for k in range(1, tp)]
    mixed = jnp.zeros((rows, skip_connection_stream.shape[1]), f32)
    for g, w in zip(others, projectors):
        mixed = mixed + jnp.dot(g, w, preferred_element_type=f32)
    first_all = (skip_connection_stream.astype(f32) + mixed).astype(jnp.bfloat16)
    normed = rms_rows(first_all, perceptron_rescaler)
    by_offset = to_offsets(normed)
    gate = joined([normed], switching)
    upper = joined(by_offset, widening)
    hidden = (jax.nn.silu(gate) * upper).astype(jnp.bfloat16)

    share = rows // tp
    parts = 2
    step = share // parts
    arrived = []
    for k in range(1, tp):
        start = ((mine + k) % tp) * share
        for i in range(parts):
            sent = jnp.dot(
                lax.dynamic_slice_in_dim(hidden, start + i * step, step, 0),
                shrinking[0],
                preferred_element_type=f32,
            ).astype(jnp.bfloat16)
            arrived.append((i, shift(sent, "tp", k)))
    own = jnp.dot(
        lax.dynamic_slice_in_dim(hidden, mine * share, share, 0),
        shrinking[0],
        preferred_element_type=f32,
    )
    first_own = lax.dynamic_slice_in_dim(first_all, mine * share, share, 0).astype(f32)
    outs = []
    for i in range(parts):
        at = slice(i * step, (i + 1) * step)
        ffn = own[at].astype(jnp.bfloat16).astype(f32)
        for j, piece in arrived:
            if j == i:
                ffn = ffn + piece.astype(f32)
        outs.append((first_own[at] + 0.5 * ffn).astype(jnp.bfloat16))
    return jnp.concatenate(outs, axis=0)


def solution(mesh):
    placed = (
        P("sp", None),
        P("sp", "tp"),
        P("sp", "tp"),
        P("sp", "tp"),
        P("sp", "tp"),
        P("sp", "tp"),
        P("tp"),
        P("sp"),
        P("sp"),
        P(),
        P("tp", None),
        P(),
        P("sp", "tp"),
        P("sp", "tp"),
        P("tp", "sp"),
    )
    return jax.shard_map(
        per_device, mesh=mesh, in_specs=placed, out_specs=P(("sp", "tp"), None), check_vma=False
    )
```
